512 devices in a mesh: fs: 16 (over y, x), tp: 32 (over z, core).
Axes of the slice: x: 4, y: 4, z: 16, core: 2. Of those that a mesh axis runs over, the one named last changes fastest.
Arguments:
- inputs: bfloat16 [6144, 2048], P('fs'), may hold values from -6 to 6
- pre_act: bfloat16 [6144, 8192], P('fs', 'tp'), may hold values from -6 to 6
- cotangent: bfloat16 [6144, 2048], P('fs'), may hold values from -6 to 6
- up_weight: bfloat16 [2048, 8192], P('fs', 'tp'), may hold values from -0.125 to 0.125
- down_weight: bfloat16 [8192, 2048], P('tp', 'fs'), may hold values from -0.0625 to 0.0625
Outputs:
- input_grad: bfloat16 [6144, 2048], P('fs')
- up_grad: float32 [2048, 8192], P('fs', 'tp')
- down_grad: float32 [8192, 2048], P('tp', 'fs')
- up_norms: float32 [2048], P('fs')
- down_norms: float32 [8192], P('tp')
The draws below stay inside these ranges and needn't reach their ends.
All inputs are finite; a program needn't handle non-finite values.
Results may differ from the reference program's by a relative error of at most 0.0051.
Values may be sent and summed in bfloat16 or wider, within the bound.
No kernel may reach another device: no remote copies, remote signals or barrier semaphores. Data moves between devices by JAX's collectives and lax.ppermute only.
A program may use at most 64 MiB of HBM per device.

```python
import jax
import jax.numpy as jnp

D = 2048
FF = 8192
TOKENS = 6144


def raised(drawn, key, source, target, shards_of, factor):
    def block_of(position):
        return (jnp.arange(drawn.shape[position]) // (drawn.shape[position] // shards_of)).reshape((-1,) + (1,) * (drawn.ndim - 1 - position))

    near = jax.random.permutation(key, shards_of)[block_of(target)]
    other_side = (block_of(target) + shards_of // 2) % shards_of
    return jnp.where((block_of(source) == near) | (block_of(source) == other_side), factor * drawn, drawn)


def steps_of(own_key, extent, cuts, low, top_value):
    def one(position, blocks):
        steps = jax.random.uniform(jax.random.fold_in(jax.random.fold_in(own_key, 6), position), (blocks,), jnp.float32, low / len(cuts), top_value / len(cuts))
        return jnp.repeat(jnp.exp(steps), extent[position] // blocks).reshape((-1,) + (1,) * (len(extent) - position - 1))

    level = one(*cuts[0])
    for cut in cuts[1:]:
        level = level * one(*cut)
    return level


def normal_values(stream_key, shape, width, most, pieces=(), held_as=jnp.bfloat16):
    entries = jax.random.normal(stream_key, shape, jnp.float32) * width
    if len(pieces) > 0:
        entries = steps_of(stream_key, shape, pieces, -0.22, 0.18) * entries
    return jnp.clip(entries, min=-most, max=most).astype(held_as)


def noise_with(own_key, dims, scale, most, cuts, heavy, held_as=jnp.bfloat16):
    result = scale * jax.random.normal(own_key, dims, jnp.float32)
    if cuts:
        result = result * steps_of(own_key, dims, cuts, -0.22, 0.18)
    return jnp.clip(raised(result, jax.random.fold_in(own_key, 3), *heavy), -most, most).astype(held_as)


def setup_inputs(seed: int = 0) -> dict:
    key_list = jax.random.split(jax.random.key(seed), 6)
    return {
        "inputs": noise_with(key_list[0], (TOKENS, D), 1.0, 6.0, ((0, 16),), (0, 1, 16, 2.0)),
        "pre_act": normal_values(key_list[1], (TOKENS, FF), 1.0, 6.0, ((0, 16), (1, 32))),
        "cotangent": noise_with(key_list[2], (TOKENS, D), 1.0, 6.0, ((0, 16),), (0, 1, 16, 2.0)),
        "up_weight": normal_values(key_list[3], (D, FF), D ** -0.5, 0.125, ((0, 16), (1, 32))),
        "down_weight": normal_values(key_list[4], (FF, D), FF ** -0.5, 0.0625, ((0, 32), (1, 16))),
    }


def reference(inputs, pre_act, cotangent, up_weight, down_weight):
    active = jnp.maximum(pre_act.astype(jnp.float32), 0.0)
    squared = (active * active).astype(jnp.bfloat16)
    sq_grad = jnp.dot(cotangent, down_weight.T, preferred_element_type=jnp.float32)
    pre_grad = (2.0 * active * sq_grad).astype(jnp.bfloat16)
    input_grad = jnp.dot(pre_grad, up_weight.T, preferred_element_type=jnp.float32).astype(jnp.bfloat16)
    up_grad = jnp.dot(inputs.T, pre_grad, preferred_element_type=jnp.float32)
    down_grad = jnp.dot(squared.T, cotangent, preferred_element_type=jnp.float32)
    up_norms = jnp.sum(up_grad * up_grad, axis=1)
    down_norms = jnp.sum(down_grad * down_grad, axis=1)
    return input_grad, up_grad, down_grad, up_norms, down_norms
```

```python
import jax
import jax.numpy as jnp
from jax import lax
from jax.sharding import Mesh
from jax.sharding import PartitionSpec as P

FS = ("y", "xh", "xl")
TP = ("zh", "zl", "core")
BF = jnp.bfloat16
F32 = jnp.float32


def from_everyone(array, axes):
    count = lax.axis_size(axes)
    return lax.all_to_all(
        jnp.broadcast_to(array[None], (count, *array.shape)), axes, 0, 0, tiled=True
    )


def exchange(array, axes):
    return lax.all_to_all(array, axes, 0, 0, tiled=True)


def other_core(array):
    return lax.ppermute(array, "core", [(0, 1), (1, 0)])


def dot(left, right, over):
    return lax.dot_general(
        left, right, ((over[:1], over[1:]), ((), ())), preferred_element_type=F32
    )


def local(inputs, pre_act, cotangent, up_weight, down_weight):
    tokens, width = inputs.shape
    hidden = pre_act.shape[1]
    core = lax.axis_index("core")
    active = jnp.maximum(pre_act.astype(F32), 0.0)
    squared = (active * active).astype(BF)

    down_columns = from_everyone(down_weight.T, FS).reshape(width, hidden)
    rows = lax.ppermute(up_weight, ("xl", "core"), [(0, 0), (1, 2), (2, 3), (3, 1)])
    up_rows = from_everyone(rows, ("xl", "y", "xh")).reshape(2, width // 2, hidden)

    sq_grad = dot(cotangent, down_columns, (1, 0))
    pre_grad = (2.0 * active * sq_grad).astype(BF)
    theirs = other_core(pre_grad)
    half = (dot(pre_grad, up_rows[0], (1, 1)) + dot(theirs, up_rows[1], (1, 1))).astype(BF)

    for axis in ("zl", "zh"):
        count = lax.axis_size(axis)
        pieces = half.reshape(count, half.shape[0] // count, half.shape[1])
        half = jnp.sum(exchange(pieces, axis).astype(F32), axis=0).astype(BF)
    half = lax.all_gather(half, "zh", axis=0, tiled=True)
    half = lax.all_gather(half, "zl", axis=0, tiled=True)
    both = other_core(half)
    first = jnp.where(core == 0, half, both).reshape(tokens, width // 256, 1, 128)
    second = jnp.where(core == 0, both, half).reshape(tokens, width // 256, 1, 128)
    input_grad = jnp.concatenate([first, second], axis=2).reshape(tokens, width)

    count = lax.axis_size(FS)
    down_part = dot(cotangent, squared, (0, 0)).astype(BF).reshape(count, width // count, hidden)
    down_grad = jnp.sum(exchange(down_part, FS).astype(F32), axis=0)
    up_part = dot(inputs, pre_grad, (0, 0)).astype(BF).reshape(count, width // count, hidden)
    up_grad = jnp.sum(exchange(up_part, FS).astype(F32), axis=0)

    down_norms = jnp.sum(from_everyone(jnp.sum(down_grad * down_grad, axis=0), FS), axis=0)
    up_norms = jnp.sum(from_everyone(jnp.sum(up_grad * up_grad, axis=1), TP), axis=0)
    return input_grad, up_grad, down_grad.T, up_norms, down_norms


def solution(mesh):
    split = Mesh(mesh.devices.reshape(4, 2, 2, 4, 4, 2), (*FS, *TP))
    return jax.shard_map(
        local,
        mesh=split,
        in_specs=(P(FS, None), P(FS, TP), P(FS, None), P(FS, TP), P(TP, FS)),
        out_specs=(P(FS, None), P(FS, TP), P(TP, FS), P(FS), P(TP)),
        check_vma=False,
    )
```

```python
import jax
import jax.numpy as jnp
from jax import lax
from jax.sharding import Mesh
from jax.sharding import PartitionSpec as P


FS = ("y", "x")
TP = ("zh", "zl", "core")
BF = jnp.bfloat16
F32 = jnp.float32


def exchange(array, axes):
    return lax.all_to_all(array, axes, 0, 0, tiled=True)


def from_everyone(array, axes):
    count = lax.axis_size(axes)
    return exchange(jnp.broadcast_to(array[None], (count, *array.shape)), axes)


def other_core(array):
    return lax.ppermute(array, "core", [(0, 1), (1, 0)])


def dot(left, right, over):
    return lax.dot_general(
        left, right, ((over[:1], over[1:]), ((), ())), preferred_element_type=F32
    )


def local(inputs, pre_act, cotangent, up_weight, down_weight):
    tokens, width = inputs.shape
    hidden = pre_act.shape[1]
    many = lax.axis_size(FS)
    part = width // many
    core = lax.axis_index("core")
    active = jnp.maximum(pre_act.astype(F32), 0.0)
    squared = (active * active).astype(BF)

    mine = jnp.concatenate([down_weight.T, up_weight], axis=0)
    weights = from_everyone(mine, FS)
    down_columns = weights[:, :part].reshape(width, hidden)
    halves = weights[:, part:].reshape(2, width // 2, hidden)
    own_rows = lax.dynamic_index_in_dim(halves, core, 0, False)
    their_rows = other_core(lax.dynamic_index_in_dim(halves, 1 - core, 0, False))
    sq_grad = dot(cotangent, down_columns, (1, 0))
    pre_grad = (2.0 * active * sq_grad).astype(BF)
    theirs = other_core(pre_grad)
    half = (dot(pre_grad, own_rows, (1, 1)) + dot(theirs, their_rows, (1, 1))).astype(BF)

    near = lax.axis_size("zl")
    pieces = exchange(half.reshape(near, tokens // near, width // 2), "zl")
    quarter = jnp.sum(pieces.astype(F32), axis=0).astype(BF)

    down_part = dot(squared, cotangent, (0, 0)).astype(BF)
    up_part = dot(pre_grad, inputs, (0, 0)).astype(BF)
    parts = jnp.concatenate([down_part, up_part], axis=0)
    parts = jnp.moveaxis(parts.reshape(2 * hidden, many, part), 1, 0)
    parts, quarter = lax.optimization_barrier((parts, quarter))
    grads = exchange(parts, FS)
    grads = jnp.sum(grads.astype(F32), axis=0)
    down_grad, up_grad = grads[:hidden], grads[hidden:]

    groups = lax.all_gather(quarter, "zh", axis=0, tiled=False)
    quarter = jnp.sum(groups.astype(F32), axis=0).astype(BF)
    up_squares = jnp.sum(up_grad * up_grad, axis=0)
    up_squares, quarter = lax.optimization_barrier((up_squares, quarter))
    up_norms = from_everyone(up_squares, TP)
    up_norms = jnp.sum(up_norms, axis=0)
    half = lax.all_gather(quarter, "zl", axis=0, tiled=True)

    down_squares = jnp.sum(down_grad * down_grad, axis=1)
    down_squares, half = lax.optimization_barrier((down_squares, half))
    down_norms = from_everyone(down_squares, FS)
    down_norms = jnp.sum(down_norms, axis=0)
    both = other_core(half)
    input_grad = jnp.concatenate(
        [jnp.where(core == 0, half, both), jnp.where(core == 0, both, half)], axis=1
    )
    return input_grad, up_grad.T, down_grad, up_norms, down_norms


def solution(mesh):
    split = Mesh(mesh.devices.reshape(4, 4, 4, 4, 2), (*FS, *TP))
    return jax.shard_map(
        local,
        mesh=split,
        in_specs=(P(FS, None), P(FS, TP), P(FS, None), P(FS, TP), P(TP, FS)),
        out_specs=(P(FS, None), P(FS, TP), P(TP, FS), P(FS), P(TP)),
        check_vma=False,
    )
```

```python
import jax
import jax.numpy as jnp
from jax import lax
from jax.sharding import Mesh
from jax.sharding import PartitionSpec as P


FS = ("yh", "yl", "x")
TP = ("zh", "zl", "core")
BF = jnp.bfloat16
F32 = jnp.float32


def exchange(array, axes):
    return lax.all_to_all(array, axes, 0, 0, tiled=True)


def from_everyone(array, axes):
    count = lax.axis_size(axes)
    return exchange(jnp.broadcast_to(array[None], (count, *array.shape)), axes)


def other_core(array):
    return lax.ppermute(array, "core", [(0, 1), (1, 0)])


def dot(left, right, over):
    return lax.dot_general(
        left, right, ((over[:1], over[1:]), ((), ())), preferred_element_type=F32
    )


def sum_near(half, axis):
    count = lax.axis_size(axis)
    here = lax.axis_index(axis)
    pieces = half.reshape(count, half.shape[0] // count, half.shape[1])
    total = lax.dynamic_index_in_dim(pieces, here, 0, False).astype(F32)
    for step in (1, 3, 2):
        there = lax.rem(here + step, count)
        piece = lax.dynamic_index_in_dim(pieces, there, 0, False)
        ring = [(i, (i + step) % count) for i in range(count)]
        total += lax.ppermute(piece, axis, ring).astype(F32)
    return total.astype(BF)


def local(inputs, pre_act, cotangent, up_weight, down_weight):
    tokens, width = inputs.shape
    hidden = pre_act.shape[1]
    many = lax.axis_size(FS)
    core = lax.axis_index("core")
    active = jnp.maximum(pre_act.astype(F32), 0.0)
    squared = (active * active).astype(BF)

    down_columns = from_everyone(down_weight.T, FS).reshape(width, hidden)
    rows = lax.ppermute(up_weight, ("yh", "core"), [(0, 0), (1, 2), (2, 3), (3, 1)])
    up_rows = from_everyone(rows, FS).reshape(2, width // 2, hidden)

    sq_grad = dot(cotangent, down_columns, (1, 0))
    pre_grad = (2.0 * active * sq_grad).astype(BF)
    theirs = other_core(pre_grad)
    half = (dot(pre_grad, up_rows[0], (1, 1)) + dot(theirs, up_rows[1], (1, 1))).astype(BF)

    down_part = dot(squared, cotangent, (0, 0)).astype(BF)
    up_part = dot(pre_grad, inputs, (0, 0)).astype(BF)
    parts = jnp.concatenate([down_part, up_part], axis=0)
    parts = jnp.moveaxis(parts.reshape(2 * hidden, many, width // many), 1, 0)
    grads = exchange(parts, FS)
    grads = jnp.sum(grads.astype(F32), axis=0)
    down_grad, up_grad = grads[:hidden], grads[hidden:]

    half = sum_near(half, "zl")
    pieces = exchange(half.reshape(4, tokens // 16, width // 2), "zh")
    half = jnp.sum(pieces.astype(F32), axis=0).astype(BF)

    up_norms = from_everyone(jnp.sum(up_grad * up_grad, axis=0), TP)
    half = lax.all_gather(half, "zh", axis=0, tiled=True)
    down_norms = from_everyone(jnp.sum(down_grad * down_grad, axis=1), FS)
    half = lax.all_gather(half, "zl", axis=0, tiled=True)
    both = other_core(half)
    input_grad = jnp.concatenate(
        [jnp.where(core == 0, half, both), jnp.where(core == 0, both, half)], axis=1
    )
    up_norms, down_norms = jnp.sum(up_norms, axis=0), jnp.sum(down_norms, axis=0)
    return input_grad, up_grad.T, down_grad, up_norms, down_norms


def solution(mesh):
    split = Mesh(mesh.devices.reshape(2, 2, 4, 4, 4, 2), (*FS, *TP))
    return jax.shard_map(
        local,
        mesh=split,
        in_specs=(P(FS, None), P(FS, TP), P(FS, None), P(FS, TP), P(TP, FS)),
        out_specs=(P(FS, None), P(FS, TP), P(TP, FS), P(FS), P(TP)),
        check_vma=False,
    )
```

```python
import jax
import jax.numpy as jnp
from jax import lax
from jax.sharding import Mesh
from jax.sharding import PartitionSpec as P


FS = ("yh", "yl", "x")
TP = ("zh", "zl", "core")
BF = jnp.bfloat16
F32 = jnp.float32


def exchange(array, axes):
    return lax.all_to_all(array, axes, 0, 0, tiled=True)


def from_everyone(array, axes):
    count = lax.axis_size(axes)
    return exchange(jnp.broadcast_to(array[None], (count, *array.shape)), axes)


def other_core(array):
    return lax.ppermute(array, "core", [(0, 1), (1, 0)])


def dot(left, right, over):
    return lax.dot_general(
        left, right, ((over[:1], over[1:]), ((), ())), preferred_element_type=F32
    )


def local(inputs, pre_act, cotangent, up_weight, down_weight):
    _, width = inputs.shape
    hidden = pre_act.shape[1]
    many = lax.axis_size(FS)
    core = lax.axis_index("core")
    active = jnp.maximum(pre_act.astype(F32), 0.0)
    squared = (active * active).astype(BF)

    down_columns = from_everyone(down_weight.T, FS).reshape(width, hidden)
    rows = lax.ppermute(up_weight, ("yh", "core"), [(0, 0), (1, 2), (2, 3), (3, 1)])
    up_rows = from_everyone(rows, FS).reshape(2, width // 2, hidden)

    sq_grad = dot(cotangent, down_columns, (1, 0))
    pre_grad = (2.0 * active * sq_grad).astype(BF)
    theirs = other_core(pre_grad)
    half = dot(pre_grad, up_rows[0], (1, 1)) + dot(theirs, up_rows[1], (1, 1))

    down_part = dot(squared, cotangent, (0, 0)).astype(BF)
    up_part = dot(pre_grad, inputs, (0, 0)).astype(BF)
    parts = jnp.concatenate([down_part, up_part], axis=0)
    parts = jnp.moveaxis(parts.reshape(2 * hidden, many, width // many), 1, 0)
    grads = exchange(parts, FS)
    grads = jnp.sum(grads.astype(F32), axis=0)
    down_grad, up_grad = grads[:hidden], grads[hidden:]

    half = lax.psum(half, ("zh", "zl")).astype(BF)
    up_norms = from_everyone(jnp.sum(up_grad * up_grad, axis=0), TP)
    down_norms = from_everyone(jnp.sum(down_grad * down_grad, axis=1), FS)
    both = other_core(half)
    input_grad = jnp.concatenate(
        [jnp.where(core == 0, half, both), jnp.where(core == 0, both, half)], axis=1
    )
    up_norms, down_norms = jnp.sum(up_norms, axis=0), jnp.sum(down_norms, axis=0)
    return input_grad, up_grad.T, down_grad, up_norms, down_norms


def solution(mesh):
    split = Mesh(mesh.devices.reshape(2, 2, 4, 4, 4, 2), (*FS, *TP))
    return jax.shard_map(
        local,
        mesh=split,
        in_specs=(P(FS, None), P(FS, TP), P(FS, None), P(FS, TP), P(TP, FS)),
        out_specs=(P(FS, None), P(FS, TP), P(TP, FS), P(FS), P(TP)),
        check_vma=False,
    )
```

```python
import jax
import jax.numpy as jnp
from jax import lax
from jax.sharding import Mesh
from jax.sharding import PartitionSpec as P


FS = ("yh", "yl", "x")
TP = ("zh", "zl", "core")
BF = jnp.bfloat16
F32 = jnp.float32


def exchange(array, axes):
    return lax.all_to_all(array, axes, 0, 0, tiled=True)


def from_everyone(array, axes):
    count = lax.axis_size(axes)
    return exchange(jnp.broadcast_to(array[None], (count, *array.shape)), axes)


def other_core(array):
    return lax.ppermute(array, "core", [(0, 1), (1, 0)])


def dot(left, right, over):
    return lax.dot_general(
        left, right, ((over[:1], over[1:]), ((), ())), preferred_element_type=F32
    )


def gather_ring(block, axes):
    count = lax.axis_size(axes)
    here = lax.axis_index(axes)
    blocks = jnp.zeros((count, *block.shape), block.dtype)
    blocks = lax.dynamic_update_index_in_dim(blocks, block, here, 0)
    for step in (1, 3, 2):
        ring = [(i, (i + step) % count) for i in range(count)]
        got = lax.ppermute(block, axes, ring)
        there = lax.rem(here + count - step, count)
        blocks = lax.dynamic_update_index_in_dim(blocks, got, there, 0)
    return blocks


def sum_at_owner(part):
    rows, width = part.shape
    many = lax.axis_size(FS)
    blocks = jnp.moveaxis(part.reshape(rows, many, width // many), 1, 0)
    return jnp.sum(exchange(blocks, FS).astype(F32), axis=0)


def local(inputs, pre_act, cotangent, up_weight, down_weight):
    _, width = inputs.shape
    hidden = pre_act.shape[1]
    core = lax.axis_index("core")
    active = jnp.maximum(pre_act.astype(F32), 0.0)
    squared = (active * active).astype(BF)

    down_columns = from_everyone(down_weight.T, FS).reshape(width, hidden)
    rows = lax.ppermute(up_weight, ("yh", "core"), [(0, 0), (1, 2), (2, 3), (3, 1)])
    rows = lax.all_gather(rows, "x", axis=0, tiled=True)
    up_rows = gather_ring(rows, ("yh", "yl")).reshape(2, width // 2, hidden)

    sq_grad = dot(cotangent, down_columns, (1, 0))
    pre_grad = (2.0 * active * sq_grad).astype(BF)
    theirs = other_core(pre_grad)
    half = dot(pre_grad, up_rows[0], (1, 1)) + dot(theirs, up_rows[1], (1, 1))

    up_grad = sum_at_owner(dot(pre_grad, inputs, (0, 0)).astype(BF))
    down_grad = sum_at_owner(dot(squared, cotangent, (0, 0)).astype(BF))

    half, up_norms = lax.psum((half, jnp.sum(up_grad * up_grad, axis=0)), ("zh", "zl"))
    half = half.astype(BF)
    up_norms += other_core(up_norms)
    down_norms = from_everyone(jnp.sum(down_grad * down_grad, axis=1), FS)
    both = other_core(half)
    input_grad = jnp.concatenate(
        [jnp.where(core == 0, half, both), jnp.where(core == 0, both, half)], axis=1
    )
    return input_grad, up_grad.T, down_grad, up_norms, jnp.sum(down_norms, axis=0)


def solution(mesh):
    split = Mesh(mesh.devices.reshape(2, 2, 4, 4, 4, 2), (*FS, *TP))
    return jax.shard_map(
        local,
        mesh=split,
        in_specs=(P(FS, None), P(FS, TP), P(FS, None), P(FS, TP), P(TP, FS)),
        out_specs=(P(FS, None), P(FS, TP), P(TP, FS), P(FS), P(TP)),
        check_vma=False,
    )
```

```python
import jax
import jax.numpy as jnp
from jax import lax
from jax.sharding import Mesh
from jax.sharding import PartitionSpec as P


FS = ("yh", "yl", "x")
TP = ("zh", "zl", "core")
BF = jnp.bfloat16
F32 = jnp.float32


def exchange(array, axes):
    return lax.all_to_all(array, axes, 0, 0, tiled=True)


def from_everyone(array, axes):
    count = lax.axis_size(axes)
    return exchange(jnp.broadcast_to(array[None], (count, *array.shape)), axes)


def other_core(array):
    return lax.ppermute(array, "core", [(0, 1), (1, 0)])


def dot(left, right, over):
    return lax.dot_general(
        left, right, ((over[:1], over[1:]), ((), ())), preferred_element_type=F32
    )


def local(inputs, pre_act, cotangent, up_weight, down_weight):
    _, width = inputs.shape
    hidden = pre_act.shape[1]
    many = lax.axis_size(FS)
    core = lax.axis_index("core")
    active = jnp.maximum(pre_act.astype(F32), 0.0)
    squared = (active * active).astype(BF)

    down_columns = from_everyone(down_weight.T, FS).reshape(width, hidden)
    rows = lax.ppermute(up_weight, ("yh", "core"), [(0, 0), (1, 2), (2, 3), (3, 1)])
    up_rows = from_everyone(rows, FS).reshape(2, width // 2, hidden)

    sq_grad = dot(cotangent, down_columns, (1, 0))
    pre_grad = (2.0 * active * sq_grad).astype(BF)
    theirs = other_core(pre_grad)
    half = dot(pre_grad, up_rows[0], (1, 1)) + dot(theirs, up_rows[1], (1, 1))

    down_part = dot(squared, cotangent, (0, 0)).astype(BF)
    up_part = dot(pre_grad, inputs, (0, 0)).astype(BF)
    parts = jnp.concatenate([down_part, up_part], axis=0)
    parts = jnp.moveaxis(parts.reshape(2 * hidden, many, width // many), 1, 0)
    grads = exchange(parts, FS)
    grads = jnp.sum(grads.astype(F32), axis=0)
    down_grad, up_grad = grads[:hidden], grads[hidden:]

    half = lax.psum(half, ("zh", "zl")).astype(BF)
    up_norms = from_everyone(jnp.sum(up_grad * up_grad, axis=0), TP)
    down_norms = lax.psum(jnp.sum(down_grad * down_grad, axis=1), ("yh", "yl"))
    down_norms = lax.psum(down_norms, "x")
    both = other_core(half)
    input_grad = jnp.concatenate(
        [jnp.where(core == 0, half, both), jnp.where(core == 0, both, half)], axis=1
    )
    up_norms = jnp.sum(up_norms, axis=0)
    return input_grad, up_grad.T, down_grad, up_norms, down_norms


def solution(mesh):
    split = Mesh(mesh.devices.reshape(2, 2, 4, 4, 4, 2), (*FS, *TP))
    return jax.shard_map(
        local,
        mesh=split,
        in_specs=(P(FS, None), P(FS, TP), P(FS, None), P(FS, TP), P(TP, FS)),
        out_specs=(P(FS, None), P(FS, TP), P(TP, FS), P(FS), P(TP)),
        check_vma=False,
    )
```

```python
import jax
import jax.numpy as jnp
from jax import lax
from jax.sharding import Mesh
from jax.sharding import PartitionSpec as P


FS = ("yh", "yl", "x")
TP = ("zh", "zl", "core")
BF = jnp.bfloat16
F32 = jnp.float32


def exchange(array, axes):
    return lax.all_to_all(array, axes, 0, 0, tiled=True)


def from_everyone(array, axes):
    count = lax.axis_size(axes)
    return exchange(jnp.broadcast_to(array[None], (count, *array.shape)), axes)


def other_core(array):
    return lax.ppermute(array, "core", [(0, 1), (1, 0)])


def dot(left, right, over):
    return lax.dot_general(
        left, right, ((over[:1], over[1:]), ((), ())), preferred_element_type=F32
    )


def both_ways(block, part):
    many = lax.axis_size(FS)
    rows, columns = block.shape
    parts = jnp.moveaxis(part.reshape(rows, many, columns), 1, 0)
    blocks = jnp.broadcast_to(block[None], parts.shape)
    got = exchange(jnp.concatenate([blocks, parts], axis=1), FS)
    return got[:, :rows], jnp.sum(got[:, rows:].astype(F32), axis=0)


def local(inputs, pre_act, cotangent, up_weight, down_weight):
    _, width = inputs.shape
    hidden = pre_act.shape[1]
    many = lax.axis_size(FS)
    core = lax.axis_index("core")
    active = jnp.maximum(pre_act.astype(F32), 0.0)
    squared = (active * active).astype(BF)

    down_part = dot(squared, cotangent, (0, 0)).astype(BF)
    down_columns, down_grad = both_ways(down_weight, down_part)
    down_columns = jnp.moveaxis(down_columns, 0, 1).reshape(hidden, width)
    sq_grad = dot(cotangent, down_columns, (1, 1))
    pre_grad = (2.0 * active * sq_grad).astype(BF)

    rows = lax.ppermute(up_weight.T, ("yh", "core"), [(0, 0), (1, 2), (2, 3), (3, 1)])
    up_part = dot(pre_grad, inputs, (0, 0)).astype(BF)
    up_rows, up_grad = both_ways(rows, up_part)
    theirs = other_core(pre_grad)
    up_rows = up_rows.reshape(2, many // 2, hidden, width // many)
    up_rows = jnp.moveaxis(up_rows, 1, 2).reshape(2, hidden, width // 2)
    half = dot(pre_grad, up_rows[0], (1, 0)) + dot(theirs, up_rows[1], (1, 0))

    down_norms = from_everyone(jnp.sum(down_grad * down_grad, axis=1), FS)
    down_norms = jnp.sum(down_norms, axis=0)
    half, up_norms = lax.psum((half, jnp.sum(up_grad * up_grad, axis=0)), ("zh", "zl"))
    half = half.astype(BF)
    up_norms += other_core(up_norms)
    both = other_core(half)
    input_grad = jnp.concatenate(
        [jnp.where(core == 0, half, both), jnp.where(core == 0, both, half)], axis=1
    )
    return input_grad, up_grad.T, down_grad, up_norms, down_norms


def solution(mesh):
    split = Mesh(mesh.devices.reshape(2, 2, 4, 4, 4, 2), (*FS, *TP))
    return jax.shard_map(
        local,
        mesh=split,
        in_specs=(P(FS, None), P(FS, TP), P(FS, None), P(FS, TP), P(TP, FS)),
        out_specs=(P(FS, None), P(FS, TP), P(TP, FS), P(FS), P(TP)),
        check_vma=False,
    )
```

```python
import jax
import jax.numpy as jnp
from jax import lax
from jax.sharding import Mesh
from jax.sharding import PartitionSpec as P


FS = ("yh", "yl", "x")
TP = ("zh", "zl", "core")
BF = jnp.bfloat16
F32 = jnp.float32


def exchange(array, axes):
    return lax.all_to_all(array, axes, 0, 0, tiled=True)


def from_everyone(array, axes):
    count = lax.axis_size(axes)
    return exchange(jnp.broadcast_to(array[None], (count, *array.shape)), axes)


def other_core(array):
    return lax.ppermute(array, "core", [(0, 1), (1, 0)])


def dot(left, right, over):
    return lax.dot_general(
        left, right, ((over[:1], over[1:]), ((), ())), preferred_element_type=F32
    )


def sum_near(half, axis):
    count = lax.axis_size(axis)
    here = lax.axis_index(axis)
    pieces = half.reshape(count, half.shape[0] // count, half.shape[1])
    total = lax.dynamic_index_in_dim(pieces, here, 0, False).astype(F32)
    for step in (1, 3, 2):
        there = lax.rem(here + step, count)
        piece = lax.dynamic_index_in_dim(pieces, there, 0, False)
        ring = [(i, (i + step) % count) for i in range(count)]
        total += lax.ppermute(piece, axis, ring).astype(F32)
    return total.astype(BF)


def local(inputs, pre_act, cotangent, up_weight, down_weight):
    _, width = inputs.shape
    hidden = pre_act.shape[1]
    many = lax.axis_size(FS)
    core = lax.axis_index("core")
    active = jnp.maximum(pre_act.astype(F32), 0.0)
    squared = (active * active).astype(BF)

    down_columns = from_everyone(down_weight.T, FS).reshape(width, hidden)
    rows = lax.ppermute(up_weight, ("yh", "core"), [(0, 0), (1, 2), (2, 3), (3, 1)])
    up_rows = from_everyone(rows, FS).reshape(2, width // 2, hidden)

    sq_grad = dot(cotangent, down_columns, (1, 0))
    pre_grad = (2.0 * active * sq_grad).astype(BF)
    theirs = other_core(pre_grad)
    half = (dot(pre_grad, up_rows[0], (1, 1)) + dot(theirs, up_rows[1], (1, 1))).astype(BF)

    down_part = dot(squared, cotangent, (0, 0)).astype(BF)
    up_part = dot(pre_grad, inputs, (0, 0)).astype(BF)
    parts = jnp.concatenate([down_part, up_part], axis=0)
    parts = jnp.moveaxis(parts.reshape(2 * hidden, many, width // many), 1, 0)
    grads = exchange(parts, FS)
    grads = jnp.sum(grads.astype(F32), axis=0)
    down_grad, up_grad = grads[:hidden], grads[hidden:]

    half = sum_near(half, "zl")
    up_norms = from_everyone(jnp.sum(up_grad * up_grad, axis=0), TP)
    groups = lax.all_gather(half, "zh", axis=0, tiled=False)
    half = jnp.sum(groups.astype(F32), axis=0).astype(BF)
    down_norms = from_everyone(jnp.sum(down_grad * down_grad, axis=1), FS)
    half = lax.all_gather(half, "zl", axis=0, tiled=True)
    both = other_core(half)
    input_grad = jnp.concatenate(
        [jnp.where(core == 0, half, both), jnp.where(core == 0, both, half)], axis=1
    )
    up_norms, down_norms = jnp.sum(up_norms, axis=0), jnp.sum(down_norms, axis=0)
    return input_grad, up_grad.T, down_grad, up_norms, down_norms


def solution(mesh):
    split = Mesh(mesh.devices.reshape(2, 2, 4, 4, 4, 2), (*FS, *TP))
    return jax.shard_map(
        local,
        mesh=split,
        in_specs=(P(FS, None), P(FS, TP), P(FS, None), P(FS, TP), P(TP, FS)),
        out_specs=(P(FS, None), P(FS, TP), P(TP, FS), P(FS), P(TP)),
        check_vma=False,
    )
```

```python
import jax
import jax.numpy as jnp
from jax import lax
from jax.sharding import Mesh
from jax.sharding import PartitionSpec as P


FS = ("yh", "yl", "x")
TP = ("zh", "zl", "core")
BF = jnp.bfloat16
EXTRA = 8
F32 = jnp.float32


def exchange(array, axes):
    return lax.all_to_all(array, axes, 0, 0, tiled=True)


def from_everyone(array, axes):
    count = lax.axis_size(axes)
    return exchange(jnp.broadcast_to(array[None], (count, *array.shape)), axes)


def other_core(array):
    return lax.ppermute(array, "core", [(0, 1), (1, 0)])


def dot(left, right, over):
    return lax.dot_general(
        left, right, ((over[:1], over[1:]), ((), ())), preferred_element_type=F32
    )


def sum_near(half, axis):
    count = lax.axis_size(axis)
    here = lax.axis_index(axis)
    pieces = half.reshape(count, half.shape[0] // count, half.shape[1])
    total = lax.dynamic_index_in_dim(pieces, here, 0, False).astype(F32)
    for step in (1, 3, 2):
        there = lax.rem(here + step, count)
        piece = lax.dynamic_index_in_dim(pieces, there, 0, False)
        ring = [(i, (i + step) % count) for i in range(count)]
        total += lax.ppermute(piece, axis, ring).astype(F32)
    return total.astype(BF)


def sum_at_owner(part):
    rows, width = part.shape
    many = lax.axis_size(FS)
    blocks = jnp.moveaxis(part.reshape(rows, many, width // many), 1, 0)
    return jnp.sum(exchange(blocks, FS).astype(F32), axis=0)


def with_row(array, values):
    high = lax.reduce_precision(values, 8, 7)
    row = jnp.concatenate([high, values - high]).astype(BF)[None]
    return jnp.concatenate(
        [array, jnp.pad(row, ((0, EXTRA - 1), (0, array.shape[1] - row.shape[1])))], axis=0
    )


def without_row(array):
    row = array[..., -EXTRA, :]
    return array[..., :-EXTRA, :], row[..., :128] + row[..., 128:256]


def local(inputs, pre_act, cotangent, up_weight, down_weight):
    tokens, width = inputs.shape
    hidden = pre_act.shape[1]
    core = lax.axis_index("core")
    active = jnp.maximum(pre_act.astype(F32), 0.0)
    squared = (active * active).astype(BF)

    down_columns = from_everyone(down_weight.T, FS).reshape(width, hidden)
    rows = lax.ppermute(up_weight, ("yh", "core"), [(0, 0), (1, 2), (2, 3), (3, 1)])
    up_rows = from_everyone(rows, FS).reshape(2, width // 2, hidden)

    sq_grad = dot(cotangent, down_columns, (1, 0))
    pre_grad = (2.0 * active * sq_grad).astype(BF)
    theirs = other_core(pre_grad)
    half = (dot(pre_grad, up_rows[0], (1, 1)) + dot(theirs, up_rows[1], (1, 1))).astype(BF)

    up_grad = sum_at_owner(dot(pre_grad, inputs, (0, 0)).astype(BF))
    down_grad = sum_at_owner(dot(squared, cotangent, (0, 0)).astype(BF))

    quarter = sum_near(half, "zl")
    quarter = with_row(quarter, jnp.sum(up_grad * up_grad, axis=0))
    groups = lax.all_gather(quarter, "zh", axis=0, tiled=False)
    quarter, squares = without_row(jnp.sum(groups.astype(F32), axis=0))
    quarter = with_row(quarter.astype(BF), squares)
    down_norms = from_everyone(jnp.sum(down_grad * down_grad, axis=1), FS)
    half = lax.all_gather(quarter, "zl", axis=0, tiled=False)
    row = half[:, -EXTRA].astype(F32)
    up_norms = jnp.sum(row[:, :128] + row[:, 128:256], axis=0)
    half = half[:, :-EXTRA].reshape(tokens, width // 2)
    both = other_core(half)
    up_norms += other_core(up_norms)
    input_grad = jnp.concatenate(
        [jnp.where(core == 0, half, both), jnp.where(core == 0, both, half)], axis=1
    )
    down_norms = jnp.sum(down_norms, axis=0)
    return input_grad, up_grad.T, down_grad, up_norms, down_norms


def solution(mesh):
    split = Mesh(mesh.devices.reshape(2, 2, 4, 4, 4, 2), (*FS, *TP))
    return jax.shard_map(
        local,
        mesh=split,
        in_specs=(P(FS, None), P(FS, TP), P(FS, None), P(FS, TP), P(TP, FS)),
        out_specs=(P(FS, None), P(FS, TP), P(TP, FS), P(FS), P(TP)),
        check_vma=False,
    )
```

```python
import jax
import jax.numpy as jnp
from jax import lax
from jax.sharding import Mesh
from jax.sharding import PartitionSpec as P


FS = ("yh", "yl", "x")
TP = ("zh", "zl", "core")
BF = jnp.bfloat16
EXTRA = 8
F32 = jnp.float32


def exchange(array, axes):
    return lax.all_to_all(array, axes, 0, 0, tiled=True)


def from_everyone(array, axes):
    count = lax.axis_size(axes)
    return exchange(jnp.broadcast_to(array[None], (count, *array.shape)), axes)


def other_core(array):
    return lax.ppermute(array, "core", [(0, 1), (1, 0)])


def dot(left, right, over):
    return lax.dot_general(
        left, right, ((over[:1], over[1:]), ((), ())), preferred_element_type=F32
    )


def sum_near(half, axis):
    count = lax.axis_size(axis)
    here = lax.axis_index(axis)
    pieces = half.reshape(count, half.shape[0] // count, half.shape[1])
    total = lax.dynamic_index_in_dim(pieces, here, 0, False).astype(F32)
    others = []
    for step in (1, 3, 2):
        there = lax.rem(here + step, count)
        piece = lax.dynamic_index_in_dim(pieces, there, 0, False)
        ring = [(i, (i + step) % count) for i in range(count)]
        others.append(lax.ppermute(piece, axis, ring))
    for other in others:
        total += other.astype(F32)
    return total.astype(BF)


def in_blocks(part):
    rows, width = part.shape
    many = lax.axis_size(FS)
    return jnp.moveaxis(part.reshape(rows, many, width // many), 1, 0)


def sum_at_owner(blocks):
    return jnp.sum(exchange(blocks, FS).astype(F32), axis=0)


def with_row(array, values):
    high = lax.reduce_precision(values, 8, 7)
    row = jnp.concatenate([high, values - high]).astype(BF)[None]
    return jnp.concatenate(
        [array, jnp.pad(row, ((0, EXTRA - 1), (0, array.shape[1] - row.shape[1])))], axis=0
    )


def without_row(array):
    row = array[..., -EXTRA, :]
    return array[..., :-EXTRA, :], row[..., :128] + row[..., 128:256]


def local(inputs, pre_act, cotangent, up_weight, down_weight):
    tokens, width = inputs.shape
    hidden = pre_act.shape[1]
    core = lax.axis_index("core")
    active = jnp.maximum(pre_act.astype(F32), 0.0)
    squared = (active * active).astype(BF)

    down_columns = from_everyone(down_weight.T, FS).reshape(width, hidden)
    rows = lax.ppermute(up_weight, ("yh", "core"), [(0, 0), (1, 2), (2, 3), (3, 1)])
    up_rows = from_everyone(rows, FS).reshape(2, width // 2, hidden)

    sq_grad = dot(cotangent, down_columns, (1, 0))
    pre_grad = (2.0 * active * sq_grad).astype(BF)
    theirs = other_core(pre_grad)
    half = (dot(pre_grad, up_rows[0], (1, 1)) + dot(theirs, up_rows[1], (1, 1))).astype(BF)

    up_grad = sum_at_owner(in_blocks(dot(pre_grad, inputs, (0, 0)).astype(BF)))
    down_part = in_blocks(dot(squared, cotangent, (0, 0)).astype(BF))
    down_grad = sum_at_owner(down_part)

    quarter = sum_near(half, "zl")
    quarter = with_row(quarter, jnp.sum(up_grad * up_grad, axis=0))
    groups = lax.all_gather(quarter, "zh", axis=0, tiled=False)
    quarter, squares = without_row(jnp.sum(groups.astype(F32), axis=0))
    quarter = with_row(quarter.astype(BF), squares)
    down_norms = from_everyone(jnp.sum(down_grad * down_grad, axis=1), FS)
    half = lax.all_gather(quarter, "zl", axis=0, tiled=False)
    row = half[:, -EXTRA].astype(F32)
    up_norms = jnp.sum(row[:, :128] + row[:, 128:256], axis=0)
    half = half[:, :-EXTRA].reshape(tokens, width // 2)
    both = other_core(half)
    up_norms += other_core(up_norms)
    input_grad = jnp.concatenate(
        [jnp.where(core == 0, half, both), jnp.where(core == 0, both, half)], axis=1
    )
    down_norms = jnp.sum(down_norms, axis=0)
    return input_grad, up_grad.T, down_grad, up_norms, down_norms


def solution(mesh):
    split = Mesh(mesh.devices.reshape(2, 2, 4, 4, 4, 2), (*FS, *TP))
    return jax.shard_map(
        local,
        mesh=split,
        in_specs=(P(FS, None), P(FS, TP), P(FS, None), P(FS, TP), P(TP, FS)),
        out_specs=(P(FS, None), P(FS, TP), P(TP, FS), P(FS), P(TP)),
        check_vma=False,
    )
```

```python
import jax
import jax.numpy as jnp
from jax import lax
from jax.sharding import Mesh
from jax.sharding import PartitionSpec as P


FS = ("yh", "yl", "x")
TP = ("zh", "zl", "core")
BF = jnp.bfloat16
EXTRA = 8
F32 = jnp.float32


def exchange(array, axes):
    return lax.all_to_all(array, axes, 0, 0, tiled=True)


def from_everyone(array, axes):
    count = lax.axis_size(axes)
    return exchange(jnp.broadcast_to(array[None], (count, *array.shape)), axes)


def other_core(array):
    return lax.ppermute(array, "core", [(0, 1), (1, 0)])


def dot(left, right, over):
    return lax.dot_general(
        left, right, ((over[:1], over[1:]), ((), ())), preferred_element_type=F32
    )


def sum_near(half, axis):
    count = lax.axis_size(axis)
    here = lax.axis_index(axis)
    pieces = half.reshape(count, half.shape[0] // count, half.shape[1])
    total = lax.dynamic_index_in_dim(pieces, here, 0, False).astype(F32)
    others = []
    for step in (1, 3, 2):
        there = lax.rem(here + step, count)
        piece = lax.dynamic_index_in_dim(pieces, there, 0, False)
        ring = [(i, (i + step) % count) for i in range(count)]
        others.append(lax.ppermute(piece, axis, ring))
    for other in others:
        total += other.astype(F32)
    return total.astype(BF)


def in_blocks(part):
    rows, width = part.shape
    many = lax.axis_size(FS)
    return jnp.moveaxis(part.reshape(rows, many, width // many), 1, 0)


def sum_at_owner(blocks):
    return jnp.sum(exchange(blocks, FS).astype(F32), axis=0)


def tile_rows(array):
    rows, columns = array.shape
    tiles = array.reshape(rows // 8, 8, columns // 128, 128)
    return jnp.swapaxes(tiles, 1, 2).reshape(-1, 128)


def from_tile_rows(tiles, columns):
    count = tiles.shape[0]
    tiles = tiles.reshape(count, -1, columns // 128, 8, 128)
    return jnp.swapaxes(tiles, 2, 3).reshape(-1, columns)


def with_row(tiles, values):
    high = lax.reduce_precision(values, 8, 7)
    rows = jnp.stack([high, values - high]).astype(BF)
    return jnp.concatenate([tiles, jnp.pad(rows, ((0, EXTRA - 2), (0, 0)))], axis=0)


def local(inputs, pre_act, cotangent, up_weight, down_weight):
    _, width = inputs.shape
    hidden = pre_act.shape[1]
    core = lax.axis_index("core")
    active = jnp.maximum(pre_act.astype(F32), 0.0)
    squared = (active * active).astype(BF)

    down_columns = from_everyone(down_weight.T, FS).reshape(width, hidden)
    rows = lax.ppermute(up_weight, ("yh", "core"), [(0, 0), (1, 2), (2, 3), (3, 1)])
    up_rows = from_everyone(rows, FS).reshape(2, width // 2, hidden)

    sq_grad = dot(cotangent, down_columns, (1, 0))
    pre_grad = (2.0 * active * sq_grad).astype(BF)
    theirs = other_core(pre_grad)
    half = (dot(pre_grad, up_rows[0], (1, 1)) + dot(theirs, up_rows[1], (1, 1))).astype(BF)

    up_grad = sum_at_owner(in_blocks(dot(pre_grad, inputs, (0, 0)).astype(BF)))
    down_part = in_blocks(dot(squared, cotangent, (0, 0)).astype(BF))
    down_grad = sum_at_owner(down_part)

    quarter = tile_rows(sum_near(half, "zl"))
    quarter = with_row(quarter, jnp.sum(up_grad * up_grad, axis=0))
    groups = lax.all_gather(quarter, "zh", axis=0, tiled=False)
    quarter = jnp.sum(groups.astype(F32), axis=0)
    squares = quarter[-EXTRA] + quarter[1 - EXTRA]
    quarter = with_row(quarter[:-EXTRA].astype(BF), squares)
    down_norms = from_everyone(jnp.sum(down_grad * down_grad, axis=1), FS)
    half = lax.all_gather(quarter, "zl", axis=0, tiled=False)
    rows = half[:, -EXTRA : 2 - EXTRA].astype(F32)
    up_norms = jnp.sum(rows, axis=(0, 1))
    half = from_tile_rows(half[:, :-EXTRA], width // 2)
    both = other_core(half)
    up_norms += other_core(up_norms)
    input_grad = jnp.concatenate(
        [jnp.where(core == 0, half, both), jnp.where(core == 0, both, half)], axis=1
    )
    down_norms = jnp.sum(down_norms, axis=0)
    return input_grad, up_grad.T, down_grad, up_norms, down_norms


def solution(mesh):
    split = Mesh(mesh.devices.reshape(2, 2, 4, 4, 4, 2), (*FS, *TP))
    return jax.shard_map(
        local,
        mesh=split,
        in_specs=(P(FS, None), P(FS, TP), P(FS, None), P(FS, TP), P(TP, FS)),
        out_specs=(P(FS, None), P(FS, TP), P(TP, FS), P(FS), P(TP)),
        check_vma=False,
    )
```

```python
import jax
import jax.numpy as jnp
from jax import lax
from jax.sharding import Mesh
from jax.sharding import PartitionSpec as P


FS = ("yh", "yl", "x")
TP = ("zh", "zl", "core")
BF = jnp.bfloat16
EXTRA = 8
F32 = jnp.float32


def exchange(array, axes):
    return lax.all_to_all(array, axes, 0, 0, tiled=True)


def from_everyone(array, axes):
    count = lax.axis_size(axes)
    return exchange(jnp.broadcast_to(array[None], (count, *array.shape)), axes)


def other_core(array):
    return lax.ppermute(array, "core", [(0, 1), (1, 0)])


def dot(left, right, over):
    return lax.dot_general(
        left, right, ((over[:1], over[1:]), ((), ())), preferred_element_type=F32
    )


def sum_near(half, axis):
    count = lax.axis_size(axis)
    here = lax.axis_index(axis)
    pieces = half.reshape(count, half.shape[0] // count, half.shape[1])
    total = lax.dynamic_index_in_dim(pieces, here, 0, False).astype(F32)
    others = []
    for step in (2, 1, 3):
        there = lax.rem(here + step, count)
        piece = lax.dynamic_index_in_dim(pieces, there, 0, False)
        ring = [(i, (i + step) % count) for i in range(count)]
        others.append(lax.ppermute(piece, axis, ring))
    for other in others:
        total += other.astype(F32)
    return total.astype(BF)


def in_blocks(part):
    rows, width = part.shape
    many = lax.axis_size(FS)
    return jnp.moveaxis(part.reshape(rows, many, width // many), 1, 0)


def sum_at_owner(blocks):
    return jnp.sum(exchange(blocks, FS).astype(F32), axis=0)


def tile_rows(array):
    rows, columns = array.shape
    tiles = array.reshape(rows // 8, 8, columns // 128, 128)
    return jnp.swapaxes(tiles, 1, 2).reshape(-1, 128)


def from_tile_rows(tiles, columns):
    count = tiles.shape[0]
    tiles = tiles.reshape(count, -1, columns // 128, 8, 128)
    return jnp.swapaxes(tiles, 2, 3).reshape(-1, columns)


def with_row(tiles, values):
    high = lax.reduce_precision(values, 8, 7)
    rows = jnp.stack([high, values - high]).astype(BF)
    return jnp.concatenate([tiles, jnp.pad(rows, ((0, EXTRA - 2), (0, 0)))], axis=0)


def local(inputs, pre_act, cotangent, up_weight, down_weight):
    _, width = inputs.shape
    hidden = pre_act.shape[1]
    core = lax.axis_index("core")
    active = jnp.maximum(pre_act.astype(F32), 0.0)
    squared = (active * active).astype(BF)

    down_columns = from_everyone(down_weight.T, FS).reshape(width, hidden)
    rows = lax.ppermute(up_weight, ("yh", "core"), [(0, 0), (1, 2), (2, 3), (3, 1)])
    up_rows = from_everyone(rows, FS).reshape(2, width // 2, hidden)

    sq_grad = dot(cotangent, down_columns, (1, 0))
    pre_grad = (2.0 * active * sq_grad).astype(BF)
    theirs = other_core(pre_grad)
    half = (dot(pre_grad, up_rows[0], (1, 1)) + dot(theirs, up_rows[1], (1, 1))).astype(BF)

    up_grad = sum_at_owner(in_blocks(dot(pre_grad, inputs, (0, 0)).astype(BF)))
    down_part = in_blocks(dot(squared, cotangent, (0, 0)).astype(BF))
    down_grad = sum_at_owner(down_part)

    quarter = tile_rows(sum_near(half, "zl"))
    quarter = with_row(quarter, jnp.sum(up_grad * up_grad, axis=0))
    groups = lax.all_gather(quarter, "zh", axis=0, tiled=False)
    quarter = jnp.sum(groups.astype(F32), axis=0)
    squares = quarter[-EXTRA] + quarter[1 - EXTRA]
    quarter = with_row(quarter[:-EXTRA].astype(BF), squares)
    down_norms = from_everyone(jnp.sum(down_grad * down_grad, axis=1), FS)
    half = lax.all_gather(quarter, "zl", axis=0, tiled=True)
    both = other_core(half)
    half, both = (each.reshape(4, -1, 128) for each in (half, both))
    rows = [each[:, -EXTRA : 2 - EXTRA].astype(F32) for each in (half, both)]
    up_norms = jnp.sum(rows[0] + rows[1], axis=(0, 1))
    half, both = (each[:, :-EXTRA] for each in (half, both))
    first = from_tile_rows(jnp.where(core == 0, half, both), width // 2)
    second = from_tile_rows(jnp.where(core == 0, both, half), width // 2)
    input_grad = jnp.concatenate([first, second], axis=1)
    down_norms = jnp.sum(down_norms, axis=0)
    return input_grad, up_grad.T, down_grad, up_norms, down_norms


def solution(mesh):
    split = Mesh(mesh.devices.reshape(2, 2, 4, 4, 4, 2), (*FS, *TP))
    return jax.shard_map(
        local,
        mesh=split,
        in_specs=(P(FS, None), P(FS, TP), P(FS, None), P(FS, TP), P(TP, FS)),
        out_specs=(P(FS, None), P(FS, TP), P(TP, FS), P(FS), P(TP)),
        check_vma=False,
    )
```

```python
import jax
import jax.numpy as jnp
from jax import lax
from jax.sharding import Mesh
from jax.sharding import PartitionSpec as P


FS = ("yh", "yl", "x")
TP = ("zh", "zl", "core")
BF = jnp.bfloat16
EXTRA = 8
F32 = jnp.float32


def exchange(array, axes):
    return lax.all_to_all(array, axes, 0, 0, tiled=True)


def from_everyone(array, axes):
    count = lax.axis_size(axes)
    return exchange(jnp.broadcast_to(array[None], (count, *array.shape)), axes)


def other_core(array):
    return lax.ppermute(array, "core", [(0, 1), (1, 0)])


def dot(left, right, over):
    return lax.dot_general(
        left, right, ((over[:1], over[1:]), ((), ())), preferred_element_type=F32
    )


def sum_near(half, axis):
    count = lax.axis_size(axis)
    here = lax.axis_index(axis)
    pieces = half.reshape(count, half.shape[0] // count, half.shape[1])
    total = lax.dynamic_index_in_dim(pieces, here, 0, False).astype(F32)
    others = []
    for step in (2, 3, 1):
        there = lax.bitwise_xor(here, step)
        piece = lax.dynamic_index_in_dim(pieces, there, 0, False)
        ring = [(i, i ^ step) for i in range(count)]
        others.append(lax.ppermute(piece, axis, ring))
    for other in others:
        total += other.astype(F32)
    return total.astype(BF)


def in_blocks(part):
    rows, width = part.shape
    many = lax.axis_size(FS)
    return jnp.moveaxis(part.reshape(rows, many, width // many), 1, 0)


def sum_at_owner(blocks):
    return jnp.sum(exchange(blocks, FS).astype(F32), axis=0)


def tile_rows(array):
    rows, columns = array.shape
    tiles = array.reshape(rows // 8, 8, columns // 128, 128)
    return jnp.swapaxes(tiles, 1, 2).reshape(-1, 128)


def from_tile_rows(tiles, columns):
    count = tiles.shape[0]
    tiles = tiles.reshape(count, -1, columns // 128, 8, 128)
    return jnp.swapaxes(tiles, 2, 3).reshape(-1, columns)


def with_row(tiles, values):
    high = lax.reduce_precision(values, 8, 7)
    rows = jnp.stack([high, values - high]).astype(BF)
    return jnp.concatenate([tiles, jnp.pad(rows, ((0, EXTRA - 2), (0, 0)))], axis=0)


def local(inputs, pre_act, cotangent, up_weight, down_weight):
    _, width = inputs.shape
    hidden = pre_act.shape[1]
    core = lax.axis_index("core")
    active = jnp.maximum(pre_act.astype(F32), 0.0)
    squared = (active * active).astype(BF)

    down_columns = from_everyone(down_weight.T, FS).reshape(width, hidden)
    rows = lax.ppermute(up_weight, ("yh", "core"), [(0, 0), (1, 2), (2, 3), (3, 1)])
    up_rows = from_everyone(rows, FS).reshape(2, width // 2, hidden)

    sq_grad = dot(cotangent, down_columns, (1, 0))
    pre_grad = (2.0 * active * sq_grad).astype(BF)
    theirs = other_core(pre_grad)
    half = (dot(pre_grad, up_rows[0], (1, 1)) + dot(theirs, up_rows[1], (1, 1))).astype(BF)

    up_grad = sum_at_owner(in_blocks(dot(pre_grad, inputs, (0, 0)).astype(BF)))
    down_part = in_blocks(dot(squared, cotangent, (0, 0)).astype(BF))
    down_grad = sum_at_owner(down_part)

    quarter = tile_rows(sum_near(half, "zl"))
    quarter = with_row(quarter, jnp.sum(up_grad * up_grad, axis=0))
    groups = lax.all_gather(quarter, "zh", axis=0, tiled=False)
    quarter = jnp.sum(groups.astype(F32), axis=0)
    squares = quarter[-EXTRA] + quarter[1 - EXTRA]
    quarter = with_row(quarter[:-EXTRA].astype(BF), squares)
    down_norms = from_everyone(jnp.sum(down_grad * down_grad, axis=1), FS)
    half = lax.all_gather(quarter, "zl", axis=0, tiled=True)
    both = other_core(half)
    half, both = (each.reshape(4, -1, 128) for each in (half, both))
    rows = [each[:, -EXTRA : 2 - EXTRA].astype(F32) for each in (half, both)]
    up_norms = jnp.sum(rows[0] + rows[1], axis=(0, 1))
    half, both = (each[:, :-EXTRA] for each in (half, both))
    first = from_tile_rows(jnp.where(core == 0, half, both), width // 2)
    second = from_tile_rows(jnp.where(core == 0, both, half), width // 2)
    input_grad = jnp.concatenate([first, second], axis=1)
    down_norms = jnp.sum(down_norms, axis=0)
    return input_grad, up_grad.T, down_grad, up_norms, down_norms


def solution(mesh):
    split = Mesh(mesh.devices.reshape(2, 2, 4, 4, 4, 2), (*FS, *TP))
    return jax.shard_map(
        local,
        mesh=split,
        in_specs=(P(FS, None), P(FS, TP), P(FS, None), P(FS, TP), P(TP, FS)),
        out_specs=(P(FS, None), P(FS, TP), P(TP, FS), P(FS), P(TP)),
        check_vma=False,
    )
```
